32 devices in a mesh: sp: 16 (over z, y, x), tp: 2 (over core).
Axes of the slice: x: 2, y: 2, z: 4, core: 2. Of those that a mesh axis runs over, the one named last changes fastest.
Arguments:
- queries: bfloat16 [4096, 8, 128], P('sp', 'tp'), may hold values from -6 to 6
- keys: bfloat16 [4096, 2, 128], P('sp'), may hold values from -6 to 6
- values: bfloat16 [4096, 2, 128], P('sp'), may hold values from -6 to 6
- documents: int32 [4096], P('sp'), may hold values from 0 to 3, never falling along the last dimension, each value on 1 to 2304 neighbouring positions
- query_gain: float32 [128], replicated, may hold values from 0.25 to 4
- key_gain: float32 [128], replicated, may hold values from 0.25 to 4
- out_weight: bfloat16 [1024, 2048], P('tp'), may hold values from -0.1875 to 0.1875
- residual: bfloat16 [4096, 2048], P('sp'), may hold values from -6 to 6
- norm_gain: float32 [2048], replicated, may hold values from 0.1 to 1.9
- up_weight: bfloat16 [2048, 6144], P('sp', 'tp'), may hold values from -0.125 to 0.125
- down_weight: bfloat16 [2048, 6144], P('sp', 'tp'), may hold values from -0.078125 to 0.078125
Outputs:
- layer_out: bfloat16 [4096, 2048], P(('sp', 'tp'))
The draws below stay inside these ranges and needn't reach their ends.
Inputs may be any that keep to these rules, and one draw needn't show every extreme that they name: `documents`: document numbers never fall along the sequence; one document covers exactly (9) * 256 positions.
All inputs are finite; a program needn't handle non-finite values.
Results may differ from the reference program's by a relative error of at most 0.017.
Values may be sent and summed in bfloat16 or wider, within the bound.
A program may use at most 128 MiB of HBM per device.

```python
import math
import jax
import jax.numpy as jnp
import numpy as np
from jax import lax

D = 2048
QUERY_HEADS = 8
KEY_VALUE_HEADS = 2
HEAD_SIZE = 128
FF = 6144
GRID = 64
TOKENS_PER_SHARD = 256
PACKED_TOKENS = 4096
N_SP = 16
N_TP = 2


def group_shared_keys(key):
    return jax.random.truncated_normal(jax.random.fold_in(key, 31), -6.0, 6.0, (PACKED_TOKENS, KEY_VALUE_HEADS, HEAD_SIZE), jnp.float32)


def draw_keys(key, part):
    return group_shared_keys(key).astype(jnp.bfloat16)


def draw_queries(key, part):
    fresh = jax.random.truncated_normal(jax.random.fold_in(key, 37), -6.0, 6.0, (PACKED_TOKENS, QUERY_HEADS, HEAD_SIZE), jnp.float32)
    return fresh.astype(jnp.bfloat16)


def draw_query_gain(key, part):
    return 1.0 + 0.18 * jax.random.truncated_normal(jax.random.fold_in(key, 43), -4.0, 4.0, (HEAD_SIZE,), jnp.float32)


def draw_key_gain(key, part):
    return 1.0 + 0.18 * jax.random.truncated_normal(jax.random.fold_in(key, 53), -4.0, 4.0, (HEAD_SIZE,), jnp.float32)


def level_of(own_key, shape, shards, least, high):
    factor_of = 1.0
    for axis_at, blocks in shards:
        steps = jax.random.uniform(jax.random.fold_in(jax.random.fold_in(own_key, 6), axis_at), (blocks,), jnp.float32, least / len(shards), high / len(shards))
        factor_of = factor_of * jnp.repeat(jnp.exp(steps), shape[axis_at] // blocks).reshape((-1,) + (1,) * (len(shape) - 1 - axis_at))
    return factor_of


def profile(number_of, total, bound, slope):
    weights = [(1 << 20) // math.isqrt(standing ** slope) + 1 for standing in range(2, number_of + 1)]
    surplus, holding = total - bound - (number_of - 1), [1] * (number_of - 1)
    while surplus > 0:
        candidates = [i for i in range(number_of - 1) if holding[i] < bound]
        mass, budget = sum([weights[i] for i in candidates]), surplus
        for i in candidates:
            addition = min(bound - holding[i], max(1, budget * weights[i] // mass), surplus)
            holding[i] = holding[i] + addition
            surplus = surplus - addition
    return np.array([bound] + holding)


def uneven_parts(key, amount, total, most, lean):
    if amount == 2:
        one = jax.random.randint(key, (), max(1, total - most), min(most, total - 1) + 1)
        return jnp.stack([one, total - one])
    lengths = jnp.asarray(profile(amount, total, most, lean), jnp.int32)
    twos = (amount - 1) // 2
    source_of, taker = lengths[1:1 + 2 * twos:2], lengths[2:2 + 2 * twos:2]
    slack = jnp.minimum(source_of - 1, most - taker)
    shifted = jax.random.randint(jax.random.fold_in(key, 1), (twos,), 0, 1 << 20) % (slack + 1)
    lengths = lengths.at[1:1 + 2 * twos:2].set(source_of - shifted).at[2:2 + 2 * twos:2].set(taker + shifted)
    return lengths[jax.random.permutation(jax.random.fold_in(key, 2), amount)]


def scatter_about(rng, shape, scale, limit, split=(), kind=jnp.bfloat16):
    drawn = jax.random.normal(rng, shape, jnp.float32) * scale
    if len(split) > 0:
        drawn = level_of(rng, shape, split, -0.22, 0.18) * drawn
    return jnp.clip(drawn, min=-limit, max=limit).astype(kind)


def setup_inputs(seed: int = 0) -> dict:
    key_of = jax.random.split(jax.random.key(seed), 12)
    return {
        "queries": draw_queries(jax.random.fold_in(key_of[11], 71), 0),
        "keys": draw_keys(jax.random.fold_in(key_of[11], 71), 0),
        "values": scatter_about(key_of[2], (PACKED_TOKENS, KEY_VALUE_HEADS, HEAD_SIZE), 1.0, 6.0, ((0, 16),)),
        "documents": jnp.searchsorted(jnp.cumsum(uneven_parts(key_of[3], N_SP // 4, PACKED_TOKENS, (N_SP // 2 + 1) * TOKENS_PER_SHARD, 0)), jnp.arange(PACKED_TOKENS), side="right").astype(jnp.int32),
        "query_gain": draw_query_gain(jax.random.fold_in(key_of[11], 71), 0),
        "key_gain": draw_key_gain(jax.random.fold_in(key_of[11], 71), 0),
        "out_weight": scatter_about(key_of[6], (QUERY_HEADS * HEAD_SIZE, D), (QUERY_HEADS * HEAD_SIZE) ** -0.5, 0.1875, ((0, 2),)),
        "residual": scatter_about(key_of[7], (PACKED_TOKENS, D), 1.0, 6.0, ((0, 16),)),
        "norm_gain": jnp.clip(1.0 + 0.18 * jax.random.normal(key_of[8], (D,), jnp.float32), 0.1, 1.9),
        "up_weight": scatter_about(key_of[9], (D, FF), D ** -0.5, 0.125, ((0, 16), (1, 2))),
        "down_weight": scatter_about(key_of[10], (D, FF), FF ** -0.5, 0.078125, ((0, 16), (1, 2))),
    }


EPS = 1e-06
THETA = 10000.0

def head_norm(block, gain):
    return block * lax.rsqrt(lax.optimization_barrier(jnp.mean(block * block, axis=-1, keepdims=True)) + EPS) * gain

def rotate(block, positions):
    head_width = block.shape[-1]
    pair_count = head_width // 4
    inverse = THETA ** (-jnp.arange(pair_count, dtype=jnp.float32) / pair_count)
    grid_row = (positions // GRID).astype(jnp.float32)[:, None] * inverse
    grid_col = (positions % GRID).astype(jnp.float32)[:, None] * inverse
    angles = jnp.concatenate([grid_row, grid_row, grid_col, grid_col], axis=-1)
    cosine = jnp.cos(angles)[:, None, :]
    sine_table = jnp.sin(angles)[:, None, :]
    turned = jnp.concatenate([-block[..., pair_count:2 * pair_count], block[..., 0:pair_count], -block[..., 3 * pair_count:], block[..., 2 * pair_count:3 * pair_count]], axis=-1)
    return block * cosine + turned * sine_table

def channel_norm(rows_in, gain):
    widened = rows_in.astype(jnp.float32)
    return (widened * lax.rsqrt(lax.optimization_barrier(jnp.mean(widened * widened, axis=-1, keepdims=True)) + EPS) * gain).astype(jnp.bfloat16)

def rounded(value):
    return lax.optimization_barrier(value.astype(jnp.bfloat16)).astype(jnp.float32)

def reference(queries, keys, values, documents, query_gain, key_gain, out_weight, residual, norm_gain, up_weight, down_weight):
    positions = jnp.arange(PACKED_TOKENS, dtype=jnp.int32)
    rotated_query = rotate(head_norm(queries.astype(jnp.float32), query_gain), positions).astype(jnp.bfloat16)
    key_rot = rotate(head_norm(keys.astype(jnp.float32), key_gain), positions).astype(jnp.bfloat16)
    query_group_count = QUERY_HEADS // KEY_VALUE_HEADS
    key_wide = key_rot.astype(jnp.float32)
    value_wide = values.astype(jnp.float32)
    query_tiles = rotated_query.reshape(N_SP, TOKENS_PER_SHARD, KEY_VALUE_HEADS, query_group_count, HEAD_SIZE)
    doc_blocks = documents.reshape(N_SP, TOKENS_PER_SHARD)
    scale = HEAD_SIZE ** (-0.5)

    def attend(item):
        query_block, doc_block = item
        scores = jnp.einsum('qgrd,kgd->grqk', query_block.astype(jnp.float32), key_wide) * scale
        allowed = (doc_block[:, None] == documents[None, :])[None, None]
        scores = jnp.where(allowed, scores, -1e+30)
        peak = lax.optimization_barrier(jnp.max(scores, axis=-1, keepdims=True))
        probs = jnp.where(allowed, jnp.exp(scores - peak), 0.0)
        denom = lax.optimization_barrier(jnp.sum(probs, axis=-1))
        summed = jnp.einsum('grqk,kgd->qgrd', rounded(probs), value_wide)
        return (summed / jnp.transpose(denom, (2, 0, 1))[..., None]).astype(jnp.bfloat16)
    attn = lax.map(attend, (query_tiles, doc_blocks)).reshape(PACKED_TOKENS, QUERY_HEADS * HEAD_SIZE)
    span = QUERY_HEADS * HEAD_SIZE // N_TP
    branch = jnp.zeros((PACKED_TOKENS, D), jnp.float32)
    for index in range(N_TP):
        partial_term = jnp.dot(attn[:, index * span:(index + 1) * span], out_weight[index * span:(index + 1) * span], preferred_element_type=jnp.float32)
        branch = branch + rounded(partial_term)
    mid = (residual.astype(jnp.float32) + branch).astype(jnp.bfloat16)
    normed = channel_norm(mid, norm_gain)
    hidden_span = FF // N_TP
    mixer = jnp.zeros((PACKED_TOKENS, D), jnp.float32)
    for index in range(N_TP):
        raised = jnp.dot(normed, up_weight[:, index * hidden_span:(index + 1) * hidden_span], preferred_element_type=jnp.float32)
        hidden = jnp.square(jax.nn.relu(raised)).astype(jnp.bfloat16)
        partial_term = lax.dot_general(hidden, down_weight[:, index * hidden_span:(index + 1) * hidden_span], (((1,), (1,)), ((), ())), preferred_element_type=jnp.float32)
        mixer = mixer + rounded(partial_term)
    return (mid.astype(jnp.float32) + mixer).astype(jnp.bfloat16)
```

```python
import functools

import jax
import jax.numpy as jnp
from jax import lax
from jax.experimental import pallas as pl
from jax.experimental.pallas import tpu as pltpu
from jax.sharding import PartitionSpec as P

QUERY_HEADS = 8
GRID = 64


EPS = 1e-06
THETA = 10000.0


def head_norm(block, gain):
    return block * lax.rsqrt(jnp.mean(block * block, axis=-1, keepdims=True) + EPS) * gain


def rotate(block, positions):
    head_width = block.shape[-1]
    pair_count = head_width // 4
    inverse = THETA ** (-jnp.arange(pair_count, dtype=jnp.float32) / pair_count)
    grid_row = (positions // GRID).astype(jnp.float32)[:, None] * inverse
    grid_col = (positions % GRID).astype(jnp.float32)[:, None] * inverse
    angles = jnp.concatenate([grid_row, grid_row, grid_col, grid_col], axis=-1)
    cosine = jnp.cos(angles)[:, None, :]
    sine_table = jnp.sin(angles)[:, None, :]
    turned = jnp.concatenate(
        [
            -block[..., pair_count : 2 * pair_count],
            block[..., 0:pair_count],
            -block[..., 3 * pair_count :],
            block[..., 2 * pair_count : 3 * pair_count],
        ],
        axis=-1,
    )
    return block * cosine + turned * sine_table


def channel_norm(rows_in, gain):
    widened = rows_in.astype(jnp.float32)
    return (
        widened * lax.rsqrt(jnp.mean(widened * widened, axis=-1, keepdims=True) + EPS) * gain
    ).astype(jnp.bfloat16)


def body(
    queries,
    keys,
    values,
    documents,
    query_gain,
    key_gain,
    out_weight,
    residual,
    norm_gain,
    up_weight,
    down_weight,
):
    tok_dev = queries.shape[0]
    heads_here = queries.shape[1]
    head_width = queries.shape[2]
    query_group_count = QUERY_HEADS // keys.shape[1]
    kv_index = lax.axis_index("tp") * heads_here // query_group_count
    positions = lax.axis_index("sp") * tok_dev + jnp.arange(tok_dev, dtype=jnp.int32)
    own_keys = lax.dynamic_index_in_dim(keys, kv_index, 1, keepdims=True)
    own_values = lax.dynamic_index_in_dim(values, kv_index, 1, keepdims=False)
    key_rot = rotate(head_norm(own_keys.astype(jnp.float32), key_gain), positions)[:, 0, :].astype(
        jnp.bfloat16
    )
    rotated_query = rotate(head_norm(queries.astype(jnp.float32), query_gain), positions).astype(
        jnp.bfloat16
    )
    scale = head_width ** (-0.5)
    first_doc = documents[0]
    last_doc = documents[tok_dev - 1]
    start_state = (
        jnp.full((tok_dev, heads_here), -1e30, jnp.float32),
        jnp.zeros((tok_dev, heads_here), jnp.float32),
        jnp.zeros((tok_dev, heads_here, head_width), jnp.float32),
    )
    piece_keys = lax.all_gather(key_rot, "sp", axis=0, tiled=True)
    piece_values = lax.all_gather(own_values, "sp", axis=0, tiled=True)
    piece_docs = lax.all_gather(documents, "sp", axis=0, tiled=True)

    def update(state):
        peak, denom, summed = state
        scores = (
            jnp.einsum("qhd,kd->qhk", rotated_query, piece_keys, preferred_element_type=jnp.float32)
            * scale
        )
        allowed = (documents[:, None] == piece_docs[None, :])[:, None, :]
        scores = jnp.where(allowed, scores, -1e30)
        new_peak = jnp.maximum(peak, jnp.max(scores, axis=-1))
        probs = jnp.where(allowed, jnp.exp(scores - new_peak[..., None]), 0.0)
        denom = jnp.sum(probs, axis=-1)
        summed = jnp.einsum(
            "qhk,kd->qhd",
            probs.astype(jnp.bfloat16),
            piece_values,
            preferred_element_type=jnp.float32,
        )
        return (new_peak, denom, summed)

    touches = jnp.logical_and(
        piece_docs[0] <= last_doc, piece_docs[piece_docs.shape[0] - 1] >= first_doc
    )
    peak, denom, summed = lax.cond(touches, update, lambda state: state, start_state)
    attn = (
        (summed / denom[..., None]).reshape(tok_dev, heads_here * head_width).astype(jnp.bfloat16)
    )
    share = tok_dev // lax.axis_size("tp")
    branch = lax.psum(
        jnp.dot(attn, out_weight, preferred_element_type=jnp.float32).astype(jnp.bfloat16), "tp"
    ).astype(jnp.float32)
    whole_rows = (residual.astype(jnp.float32) + branch).astype(jnp.bfloat16)
    normed = channel_norm(whole_rows, norm_gain)
    mid = lax.dynamic_slice_in_dim(whole_rows, lax.axis_index("tp") * share, share, 0)
    raised = jnp.dot(
        normed,
        lax.all_gather(up_weight, "sp", axis=0, tiled=True),
        preferred_element_type=jnp.float32,
    )
    hidden = jnp.square(jax.nn.relu(raised)).astype(jnp.bfloat16)
    terms = lax.dot_general(
        hidden,
        lax.all_gather(down_weight, "sp", axis=0, tiled=True),
        (((1,), (1,)), ((), ())),
        preferred_element_type=jnp.float32,
    )
    mixer = lax.psum_scatter(
        terms.astype(jnp.bfloat16), "tp", scatter_dimension=0, tiled=True
    ).astype(jnp.float32)
    return (mid.astype(jnp.float32) + mixer).astype(jnp.bfloat16)


MESH = pl.DeviceIdType.MESH
NT = (((1,), (1,)), ((), ()))
F32 = jnp.float32
BF16 = jnp.bfloat16


def layer_kernel(
    q_ref, kv_ref, drow_ref, dcol_ref, ow_ref, res_ref, gain_ref, up_ref, down_ref, out_ref,
    kv_all, doc_all, attn, wup, wdown, part, part_in, mid, norm_all, hidden, outs, outs_in, sums,
    final_in, kv_s, kv_r, dc_s, dc_r, w_s, w_r, loc_s, p_s, p_r, n_s, n_r, o_s, o_r, f_s, f_r,
):
    heads, rows, width = q_ref.shape
    half = rows // 2
    depth, cols = wup.shape[1], wup.shape[2]
    model = ow_ref.shape[1]
    sp, core = lax.axis_index("sp"), lax.axis_index("tp")
    n_z = lax.axis_size("sp") // 4
    x, y, z = sp % 2, (sp // 2) % 2, sp // 4

    def at(dx, dy, r):
        return ((z + r) % n_z * 2 + (y + dy) % 2) * 2 + (x + dx) % 2

    def mate(rc):
        return (((z // 2) * 2 + (z + rc // 2) % 2) * 2 + y) * 2 + (x + rc) % 2

    def rank(spi):
        return (spi // 4) % 2 * 2 + spi % 2

    sent = []

    def send(src, dst, ss, rs, spi, tpi):
        c = pltpu.make_async_remote_copy(
            src_ref=src, dst_ref=dst, send_sem=ss, recv_sem=rs,
            device_id=(spi, tpi), device_id_type=MESH,
        )
        c.start()
        sent.append(c)

    def arrive(dst, ss, rs):
        pltpu.make_async_remote_copy(
            src_ref=dst, dst_ref=dst, send_sem=ss, recv_sem=rs,
            device_id=(sp, 1 - core), device_id_type=MESH,
        ).wait_recv()

    barrier = pltpu.get_barrier_semaphore()
    peers = [(at(dx, 0, k), core) for dx in (0, 1) for k in range(n_z) if dx or k]
    peers += [(at(0, 1, 0), core), (sp, 1 - core)]
    for p in peers:
        pl.semaphore_signal(barrier, inc=1, device_id=p, device_id_type=MESH)
    pl.semaphore_wait(barrier, len(peers))

    def slot(dx, dy, r):
        return (dx * 2 + dy) * n_z + r

    def send_kv(src_slot, dst_slot, spi):
        src = kv_ref if src_slot is None else kv_all.at[src_slot]
        dsrc = drow_ref if src_slot is None else doc_all.at[src_slot]
        i = dst_slot
        send(src, kv_all.at[dst_slot], kv_s.at[i], kv_r.at[i], spi, core)
        send(dsrc, doc_all.at[dst_slot], dc_s.at[i], dc_r.at[i], spi, core)

    def wait_kv(i):
        arrive(kv_all.at[i], kv_s.at[i], kv_r.at[i])
        arrive(doc_all.at[i], dc_s.at[i], dc_r.at[i])

    weights = ((up_ref, wup), (down_ref, wdown))

    def send_weight(w, dx, k):
        src, dst = weights[w]
        target = at(dx, 0, k)
        block = src.at[:, pl.ds(pl.multiple_of(rank(target) * cols, 128), cols)]
        i = dx * n_z + (n_z - k) % n_z
        if dx or k:
            send(block, dst.at[sp], w_s.at[w, i], w_r.at[w, i], target, core)

    def forward_weight(w, i):
        dst = weights[w][1]
        owner = at(i // n_z, 0, i % n_z)
        if i:
            arrive(dst.at[owner], w_s.at[w, i], w_r.at[w, i])
        j = 2 * n_z + i
        send(dst.at[owner], dst.at[owner], w_s.at[w, j], w_r.at[w, j], at(0, 1, 0), core)

    def last_weight(w):
        dst = weights[w][1]
        for i in range(2 * n_z):
            owner = at(i // n_z, 1, i % n_z)
            arrive(dst.at[owner], w_s.at[w, 2 * n_z + i], w_r.at[w, 2 * n_z + i])

    for k in range(1, n_z):
        send_kv(None, slot(0, 0, n_z - k), at(0, 0, k))
    send_kv(None, slot(1, 0, 0), at(1, 0, 0))
    send_kv(None, slot(0, 1, 0), at(0, 1, 0))
    own = []
    for w in (0, 1):
        src, dst = weights[w]
        block = src.at[:, pl.ds(pl.multiple_of(rank(sp) * cols, 128), cols)]
        own.append(pltpu.make_async_copy(block, dst.at[sp], loc_s.at[w]))
    own.append(pltpu.make_async_copy(kv_ref, kv_all.at[0], loc_s.at[2]))
    own.append(pltpu.make_async_copy(drow_ref, doc_all.at[0], loc_s.at[3]))
    for c in own:
        c.start()
    near = sorted(range(1, n_z), key=lambda r: min(r, n_z - r))
    for k in near:
        send_weight(0, 0, k)
    for r in near:
        wait_kv(slot(0, 0, r))
        send_kv(slot(0, 0, r), slot(1, 0, r), at(1, 0, 0))
        send_kv(slot(0, 0, r), slot(0, 1, r), at(0, 1, 0))
    for r in [0] + near:
        wait_kv(slot(1, 0, r))
        if r < n_z // 2:
            send_kv(slot(1, 0, r), slot(1, 1, r), at(0, 1, 0))
        wait_kv(slot(0, 1, r))
        if r >= n_z // 2:
            send_kv(slot(0, 1, r), slot(1, 1, r), at(1, 0, 0))
    for c in own:
        c.wait()
    for k in [0] + near:
        send_weight(0, 1, k)
    for k in near:
        send_weight(1, 0, k)
    for k in [0] + near:
        send_weight(1, 1, k)
    order = [dx * n_z + r for dx in (0, 1) for r in [0] + near]
    forward_weight(0, order[0])
    for r in range(n_z):
        wait_kv(slot(1, 1, r))

    scale = width ** (-0.5)
    n_slots = kv_all.shape[0]
    todo = order[1:]
    for h in range(heads):

        def step(i, state):
            peak, denom, acc = state
            scores = lax.dot_general(q_ref[h], kv_all[i, 0], NT, preferred_element_type=F32) * scale
            allowed = dcol_ref[...] == doc_all[i]
            scores = jnp.where(allowed, scores, -1e30)
            new_peak = jnp.maximum(peak, jnp.max(scores, axis=-1, keepdims=True))
            probs = jnp.where(allowed, jnp.exp(scores - new_peak), 0.0)
            decay = jnp.exp(peak - new_peak)
            denom = denom * decay + jnp.sum(probs, axis=-1, keepdims=True)
            acc = acc * decay + jnp.dot(
                probs.astype(BF16), kv_all[i, 1], preferred_element_type=F32
            )
            return new_peak, denom, acc

        state = (
            jnp.full((rows, 1), -1e30, F32),
            jnp.zeros((rows, 1), F32),
            jnp.zeros((rows, width), F32),
        )
        peak, denom, acc = lax.fori_loop(0, n_slots, step, state)
        attn[:, h * width : (h + 1) * width] = (acc / denom).astype(BF16)
        if h >= heads // 2:
            for i in todo[:2]:
                forward_weight(0, i)
            todo = todo[2:]

    tile = 256

    @pl.loop(0, model // tile)
    def _(t):
        lanes = pl.ds(pl.multiple_of(t * tile, tile), tile)
        p = jnp.dot(attn[...], ow_ref[:, lanes], preferred_element_type=F32).astype(BF16)
        part[0, :, lanes] = p[:half]
        part[1, :, lanes] = p[half:]

    send(part.at[1 - core], part_in, p_s, p_r, sp, 1 - core)
    arrive(part_in, p_s, p_r)
    start = pl.ds(pl.multiple_of(core * half, half), half)
    group = 32

    @pl.loop(0, half // group)
    def _(t):
        rws = pl.ds(pl.multiple_of(t * group, group), group)
        branch = part[core, rws].astype(F32) + part_in[rws].astype(F32)
        rres = pl.ds(pl.multiple_of(core * half + t * group, group), group)
        m = (res_ref[rres].astype(F32) + branch).astype(BF16)
        mid[rws] = m
        wide = m.astype(F32)
        inv = lax.rsqrt(jnp.mean(wide * wide, axis=-1, keepdims=True) + EPS)
        norm_all[0, 0, rws] = (wide * inv * gain_ref[...]).astype(BF16)

    for rc in (3, 1, 2):
        send(norm_all.at[0, 0], norm_all.at[rc, 0], n_s.at[rc], n_r.at[rc], mate(rc), core)
    send(norm_all.at[0, 0], norm_all.at[0, 1], n_s.at[4], n_r.at[4], sp, 1 - core)
    for i in todo:
        forward_weight(0, i)
    for i in order[:1] + order[1:5]:
        forward_weight(1, i)
    for rc in (1, 2, 3):
        arrive(norm_all.at[rc, 0], n_s.at[rc], n_r.at[rc])
        j = 4 + rc
        send(norm_all.at[rc, 0], norm_all.at[rc, 1], n_s.at[j], n_r.at[j], sp, 1 - core)
    for i in order[5:]:
        forward_weight(1, i)
    last_weight(0)
    for rc in range(4):
        arrive(norm_all.at[rc, 1], n_s.at[4 + rc], n_r.at[4 + rc])

    @pl.loop(0, 4 * (cols // tile))
    def _(t):
        rc, c = t // (cols // tile), t % (cols // tile)
        lanes = pl.ds(pl.multiple_of(c * tile, tile), tile)
        tokens = norm_all[rc].reshape(rows, model)
        w = wup[:, :, lanes].reshape(model, tile)
        raised = jnp.dot(tokens, w, preferred_element_type=F32)
        hidden[rc, :, lanes] = jnp.square(jnp.maximum(raised, 0.0)).astype(BF16)

    last_weight(1)
    blocks = tile // depth

    for rc in (3, 1, 2, 0):

        @pl.loop(0, model // tile)
        def _(t):
            lanes = pl.ds(pl.multiple_of(t * tile, tile), tile)
            w = wdown[pl.ds(t * blocks, blocks)].reshape(tile, cols)
            o = lax.dot_general(hidden[rc], w, NT, preferred_element_type=F32).astype(BF16)
            outs[rc, 0, :, lanes] = o[:half]
            outs[rc, 1, :, lanes] = o[half:]

        send(outs.at[rc, 1], outs_in.at[rc], o_s.at[rc], o_r.at[rc], sp, 1 - core)

    for rc in (3, 1, 2, 0):
        arrive(outs_in.at[rc], o_s.at[rc], o_r.at[rc])
        if rc:

            @pl.loop(0, half // group)
            def _(t):
                rws = pl.ds(pl.multiple_of(t * group, group), group)
                sums[rc - 1, rws] = (
                    outs[rc, 0, rws].astype(F32) + outs_in[rc, rws].astype(F32)
                ).astype(BF16)

            send(sums.at[rc - 1], final_in.at[rc - 1], f_s.at[rc], f_r.at[rc], mate(rc), core)
    for rc in (1, 2, 3):
        arrive(final_in.at[rc - 1], f_s.at[rc], f_r.at[rc])

    @pl.loop(0, half // group)
    def _(t):
        rws = pl.ds(pl.multiple_of(t * group, group), group)
        total = outs[0, 0, rws].astype(F32) + outs_in[0, rws].astype(F32)
        for rc in range(3):
            total += final_in[rc, rws].astype(F32)
        out_ref[rws] = (mid[rws].astype(F32) + total).astype(BF16)

    for c in sent:
        c.wait_send()


def fused_body(
    queries, keys, values, documents, query_gain, key_gain, out_weight, residual, norm_gain,
    up_weight, down_weight,
):
    rows, heads, width = queries.shape
    n_sp = lax.axis_size("sp")
    model = residual.shape[1]
    depth, cols = up_weight.shape[0], up_weight.shape[1] // 4
    half = rows // 2
    kv_index = lax.axis_index("tp") * heads // (QUERY_HEADS // keys.shape[1])
    positions = lax.axis_index("sp") * rows + jnp.arange(rows, dtype=jnp.int32)
    own_keys = lax.dynamic_index_in_dim(keys, kv_index, 1, keepdims=True)
    own_values = lax.dynamic_index_in_dim(values, kv_index, 1, keepdims=False)
    key_rot = rotate(head_norm(own_keys.astype(F32), key_gain), positions)[:, 0, :].astype(BF16)
    query_rot = rotate(head_norm(queries.astype(F32), query_gain), positions).astype(BF16)
    vm = pl.BlockSpec(memory_space=pltpu.VMEM)
    dma = pltpu.SemaphoreType.DMA
    token = (half, model)
    return pl.pallas_call(
        layer_kernel,
        out_shape=jax.ShapeDtypeStruct(token, BF16),
        in_specs=[vm] * 9,
        out_specs=vm,
        scratch_shapes=[
            pltpu.VMEM((n_sp, 2, rows, width), BF16),
            pltpu.VMEM((n_sp, 1, rows), jnp.int32),
            pltpu.VMEM((rows, heads * width), BF16),
            pltpu.VMEM((n_sp, depth, cols), BF16),
            pltpu.VMEM((n_sp, depth, cols), BF16),
            pltpu.VMEM((2,) + token, BF16),
            pltpu.VMEM(token, BF16),
            pltpu.VMEM(token, BF16),
            pltpu.VMEM((4, 2) + token, BF16),
            pltpu.VMEM((4, rows, cols), BF16),
            pltpu.VMEM((4, 2) + token, BF16),
            pltpu.VMEM((4,) + token, BF16),
            pltpu.VMEM((3,) + token, BF16),
            pltpu.VMEM((3,) + token, BF16),
            dma((n_sp,)), dma((n_sp,)), dma((n_sp,)), dma((n_sp,)),
            dma((2, n_sp)), dma((2, n_sp)), dma((4,)),
            dma, dma, dma((8,)), dma((8,)), dma((4,)), dma((4,)), dma((4,)), dma((4,)),
        ],
        compiler_params=pltpu.CompilerParams(
            collective_id=0, has_side_effects=True, vmem_limit_bytes=60 * 1024 * 1024
        ),
    )(
        query_rot.transpose(1, 0, 2),
        jnp.stack([key_rot, own_values]),
        documents[None, :],
        documents[:, None],
        out_weight,
        residual,
        norm_gain[None, :],
        up_weight,
        down_weight,
    )


def solution(mesh):
    in_specs = (
        P("sp", "tp", None),
        P("sp", None, None),
        P("sp", None, None),
        P("sp"),
        P(),
        P(),
        P("tp", None),
        P("sp", None),
        P(),
        P("sp", "tp"),
        P("sp", "tp"),
    )
    out_specs = P(("sp", "tp"), None)
    fused = mesh.shape["tp"] == 2 and mesh.shape["sp"] == 16
    return jax.shard_map(fused_body if fused else body, mesh=mesh, in_specs=in_specs, out_specs=out_specs, check_vma=False)
```

```python
import functools

import jax
import jax.numpy as jnp
from jax import lax
from jax.experimental import pallas as pl
from jax.experimental.pallas import tpu as pltpu
from jax.sharding import PartitionSpec as P

QUERY_HEADS = 8
GRID = 64


EPS = 1e-06
THETA = 10000.0


def head_norm(block, gain):
    return block * lax.rsqrt(jnp.mean(block * block, axis=-1, keepdims=True) + EPS) * gain


def rotate(block, positions):
    head_width = block.shape[-1]
    pair_count = head_width // 4
    inverse = THETA ** (-jnp.arange(pair_count, dtype=jnp.float32) / pair_count)
    grid_row = (positions // GRID).astype(jnp.float32)[:, None] * inverse
    grid_col = (positions % GRID).astype(jnp.float32)[:, None] * inverse
    angles = jnp.concatenate([grid_row, grid_row, grid_col, grid_col], axis=-1)
    cosine = jnp.cos(angles)[:, None, :]
    sine_table = jnp.sin(angles)[:, None, :]
    turned = jnp.concatenate(
        [
            -block[..., pair_count : 2 * pair_count],
            block[..., 0:pair_count],
            -block[..., 3 * pair_count :],
            block[..., 2 * pair_count : 3 * pair_count],
        ],
        axis=-1,
    )
    return block * cosine + turned * sine_table


def channel_norm(rows_in, gain):
    widened = rows_in.astype(jnp.float32)
    return (
        widened * lax.rsqrt(jnp.mean(widened * widened, axis=-1, keepdims=True) + EPS) * gain
    ).astype(jnp.bfloat16)


def body(
    queries,
    keys,
    values,
    documents,
    query_gain,
    key_gain,
    out_weight,
    residual,
    norm_gain,
    up_weight,
    down_weight,
):
    tok_dev = queries.shape[0]
    heads_here = queries.shape[1]
    head_width = queries.shape[2]
    query_group_count = QUERY_HEADS // keys.shape[1]
    kv_index = lax.axis_index("tp") * heads_here // query_group_count
    positions = lax.axis_index("sp") * tok_dev + jnp.arange(tok_dev, dtype=jnp.int32)
    own_keys = lax.dynamic_index_in_dim(keys, kv_index, 1, keepdims=True)
    own_values = lax.dynamic_index_in_dim(values, kv_index, 1, keepdims=False)
    key_rot = rotate(head_norm(own_keys.astype(jnp.float32), key_gain), positions)[:, 0, :].astype(
        jnp.bfloat16
    )
    rotated_query = rotate(head_norm(queries.astype(jnp.float32), query_gain), positions).astype(
        jnp.bfloat16
    )
    scale = head_width ** (-0.5)
    first_doc = documents[0]
    last_doc = documents[tok_dev - 1]
    start_state = (
        jnp.full((tok_dev, heads_here), -1e30, jnp.float32),
        jnp.zeros((tok_dev, heads_here), jnp.float32),
        jnp.zeros((tok_dev, heads_here, head_width), jnp.float32),
    )
    piece_keys = lax.all_gather(key_rot, "sp", axis=0, tiled=True)
    piece_values = lax.all_gather(own_values, "sp", axis=0, tiled=True)
    piece_docs = lax.all_gather(documents, "sp", axis=0, tiled=True)

    def update(state):
        peak, denom, summed = state
        scores = (
            jnp.einsum("qhd,kd->qhk", rotated_query, piece_keys, preferred_element_type=jnp.float32)
            * scale
        )
        allowed = (documents[:, None] == piece_docs[None, :])[:, None, :]
        scores = jnp.where(allowed, scores, -1e30)
        new_peak = jnp.maximum(peak, jnp.max(scores, axis=-1))
        probs = jnp.where(allowed, jnp.exp(scores - new_peak[..., None]), 0.0)
        denom = jnp.sum(probs, axis=-1)
        summed = jnp.einsum(
            "qhk,kd->qhd",
            probs.astype(jnp.bfloat16),
            piece_values,
            preferred_element_type=jnp.float32,
        )
        return (new_peak, denom, summed)

    touches = jnp.logical_and(
        piece_docs[0] <= last_doc, piece_docs[piece_docs.shape[0] - 1] >= first_doc
    )
    peak, denom, summed = lax.cond(touches, update, lambda state: state, start_state)
    attn = (
        (summed / denom[..., None]).reshape(tok_dev, heads_here * head_width).astype(jnp.bfloat16)
    )
    share = tok_dev // lax.axis_size("tp")
    branch = lax.psum(
        jnp.dot(attn, out_weight, preferred_element_type=jnp.float32).astype(jnp.bfloat16), "tp"
    ).astype(jnp.float32)
    whole_rows = (residual.astype(jnp.float32) + branch).astype(jnp.bfloat16)
    normed = channel_norm(whole_rows, norm_gain)
    mid = lax.dynamic_slice_in_dim(whole_rows, lax.axis_index("tp") * share, share, 0)
    raised = jnp.dot(
        normed,
        lax.all_gather(up_weight, "sp", axis=0, tiled=True),
        preferred_element_type=jnp.float32,
    )
    hidden = jnp.square(jax.nn.relu(raised)).astype(jnp.bfloat16)
    terms = lax.dot_general(
        hidden,
        lax.all_gather(down_weight, "sp", axis=0, tiled=True),
        (((1,), (1,)), ((), ())),
        preferred_element_type=jnp.float32,
    )
    mixer = lax.psum_scatter(
        terms.astype(jnp.bfloat16), "tp", scatter_dimension=0, tiled=True
    ).astype(jnp.float32)
    return (mid.astype(jnp.float32) + mixer).astype(jnp.bfloat16)


MESH = pl.DeviceIdType.MESH
NT = (((1,), (1,)), ((), ()))
F32 = jnp.float32
BF16 = jnp.bfloat16
LOG2E = 1.4426950408889634
APART = 1024.0


def layer_kernel(
    q_ref, key_ref, val_ref, ow_ref, res_ref, gain_ref, up_ref, down_ref, out_ref,
    key_all, val_all, attn, wup, wdown, part, part_in, mid, norm_all, hidden, outs, outs_in, sums,
    final_in, kv_s, kv_r, dc_s, dc_r, w_s, w_r, loc_s, p_s, p_r, n_s, n_r, o_s, o_r, f_s, f_r,
):
    heads, rows = q_ref.shape[:2]
    used, width = key_ref.shape[0], val_ref.shape[1]
    half = rows // 2
    depth, cols = wup.shape[1], wup.shape[2]
    model = ow_ref.shape[1]
    sp, core = lax.axis_index("sp"), lax.axis_index("tp")
    n_z = lax.axis_size("sp") // 4
    x, y, z = sp % 2, (sp // 2) % 2, sp // 4

    def at(dx, dy, r):
        return ((z + r) % n_z * 2 + (y + dy) % 2) * 2 + (x + dx) % 2

    def mate(rc):
        return (((z // 2) * 2 + (z + rc // 2) % 2) * 2 + y) * 2 + (x + rc) % 2

    def rank(spi):
        return (spi // 4) % 2 * 2 + spi % 2

    sent = []

    def send(src, dst, ss, rs, spi, tpi):
        c = pltpu.make_async_remote_copy(
            src_ref=src, dst_ref=dst, send_sem=ss, recv_sem=rs,
            device_id=(spi, tpi), device_id_type=MESH,
        )
        c.start()
        sent.append(c)

    def arrive(dst, ss, rs):
        pltpu.make_async_remote_copy(
            src_ref=dst, dst_ref=dst, send_sem=ss, recv_sem=rs,
            device_id=(sp, 1 - core), device_id_type=MESH,
        ).wait_recv()

    barrier = pltpu.get_barrier_semaphore()
    peers = [(at(dx, 0, k), core) for dx in (0, 1) for k in range(n_z) if dx or k]
    peers += [(at(0, 1, 0), core), (sp, 1 - core)]
    for p in peers:
        pl.semaphore_signal(barrier, inc=1, device_id=p, device_id_type=MESH)
    pl.semaphore_wait(barrier, len(peers))

    def slot(dx, dy, r):
        return (dx * 2 + dy) * n_z + r

    def key_at(i):
        return key_all.at[i, pl.ds(0, used)]

    def val_at(i):
        return val_all.at[i, :, pl.ds(0, width)]

    def send_kv(src_slot, i, spi):
        ksrc = key_ref if src_slot is None else key_at(src_slot)
        vsrc = val_ref if src_slot is None else val_at(src_slot)
        send(ksrc, key_at(i), kv_s.at[i], kv_r.at[i], spi, core)
        send(vsrc, val_at(i), dc_s.at[i], dc_r.at[i], spi, core)

    def wait_kv(i):
        arrive(key_at(i), kv_s.at[i], kv_r.at[i])
        arrive(val_at(i), dc_s.at[i], dc_r.at[i])

    weights = ((up_ref, wup), (down_ref, wdown))

    def send_weight(w, dx, k):
        src, dst = weights[w]
        target = at(dx, 0, k)
        block = src.at[:, pl.ds(pl.multiple_of(rank(target) * cols, 128), cols)]
        i = dx * n_z + (n_z - k) % n_z
        if dx or k:
            send(block, dst.at[sp], w_s.at[w, i], w_r.at[w, i], target, core)

    def forward_weight(w, i):
        dst = weights[w][1]
        owner = at(i // n_z, 0, i % n_z)
        if i:
            arrive(dst.at[owner], w_s.at[w, i], w_r.at[w, i])
        j = 2 * n_z + i
        send(dst.at[owner], dst.at[owner], w_s.at[w, j], w_r.at[w, j], at(0, 1, 0), core)

    def last_weight(w):
        dst = weights[w][1]
        for i in range(2 * n_z):
            owner = at(i // n_z, 1, i % n_z)
            arrive(dst.at[owner], w_s.at[w, 2 * n_z + i], w_r.at[w, 2 * n_z + i])

    for k in range(1, n_z):
        send_kv(None, slot(0, 0, n_z - k), at(0, 0, k))
    send_kv(None, slot(1, 0, 0), at(1, 0, 0))
    send_kv(None, slot(0, 1, 0), at(0, 1, 0))
    own = []
    for w in (0, 1):
        src, dst = weights[w]
        block = src.at[:, pl.ds(pl.multiple_of(rank(sp) * cols, 128), cols)]
        own.append(pltpu.make_async_copy(block, dst.at[sp], loc_s.at[w]))
    own.append(pltpu.make_async_copy(key_ref, key_at(0), loc_s.at[2]))
    own.append(pltpu.make_async_copy(val_ref, val_at(0), loc_s.at[3]))
    for c in own:
        c.start()
    order = [dx * n_z + r for dx in (0, 1) for r in (0, 1, n_z - 1, *range(2, n_z - 1))]
    near = sorted(range(1, n_z), key=lambda r: min(r, n_z - r))
    for k in near:
        send_weight(0, 0, k)
    n_slots = key_all.shape[0]

    @pl.loop(0, n_slots)
    def _(i):
        key_all[i, used:, :] = jnp.zeros((key_all.shape[1] - used, rows), BF16)
        val_all[i, :, width:] = jnp.ones((rows, val_all.shape[2] - width), BF16)

    for r in near:
        wait_kv(slot(0, 0, r))
        send_kv(slot(0, 0, r), slot(1, 0, r), at(1, 0, 0))
        send_kv(slot(0, 0, r), slot(0, 1, r), at(0, 1, 0))
    for r in [0] + near:
        wait_kv(slot(1, 0, r))
        if r < n_z // 2:
            send_kv(slot(1, 0, r), slot(1, 1, r), at(0, 1, 0))
        wait_kv(slot(0, 1, r))
        if r >= n_z // 2:
            send_kv(slot(0, 1, r), slot(1, 1, r), at(1, 0, 0))
    for c in own:
        c.wait()
    for k in [0] + near:
        send_weight(0, 1, k)
    for k in near:
        send_weight(1, 0, k)
    for i in order[:3]:
        forward_weight(0, i)
    for r in range(n_z):
        wait_kv(slot(1, 1, r))

    todo = order[3:]
    span = 4
    for h in range(heads):

        def step(g, state):
            peak, acc = state
            scores = [
                jnp.dot(q_ref[h], key_all[g * span + j], preferred_element_type=F32)
                for j in range(span)
            ]
            highest = functools.reduce(jnp.maximum, scores)
            new_peak = jnp.maximum(peak, jnp.max(highest, axis=-1, keepdims=True))
            acc = acc * jnp.exp2(peak - new_peak)
            for j in range(span):
                probs = jnp.exp2(scores[j] - new_peak).astype(BF16)
                acc += jnp.dot(probs, val_all[g * span + j], preferred_element_type=F32)
            return new_peak, acc

        state = (jnp.full((rows, 1), -1e30, F32), jnp.zeros((rows, 2 * width), F32))
        _, acc = lax.fori_loop(0, n_slots // span, step, state)
        attn[:, h * width : (h + 1) * width] = (acc[:, :width] / acc[:, width:]).astype(BF16)
        for i in todo[:1]:
            forward_weight(0, i)
        todo = todo[1:]

    tile = 256

    @pl.loop(0, model // tile)
    def _(t):
        lanes = pl.ds(pl.multiple_of(t * tile, tile), tile)
        p = jnp.dot(attn[...], ow_ref[:, lanes], preferred_element_type=F32).astype(BF16)
        part[0, :, lanes] = p[:half]
        part[1, :, lanes] = p[half:]

    send(part.at[1 - core], part_in, p_s, p_r, sp, 1 - core)
    arrive(part_in, p_s, p_r)
    start = pl.ds(pl.multiple_of(core * half, half), half)
    group = 32

    @pl.loop(0, half // group)
    def _(t):
        rws = pl.ds(pl.multiple_of(t * group, group), group)
        branch = part[core, rws].astype(F32) + part_in[rws].astype(F32)
        rres = pl.ds(pl.multiple_of(core * half + t * group, group), group)
        m = (res_ref[rres].astype(F32) + branch).astype(BF16)
        mid[rws] = m
        wide = m.astype(F32)
        inv = lax.rsqrt(jnp.mean(wide * wide, axis=-1, keepdims=True) + EPS)
        norm_all[0, 0, rws] = (wide * inv * gain_ref[...]).astype(BF16)

    for rc in (3, 1, 2):
        send(norm_all.at[0, 0], norm_all.at[rc, 0], n_s.at[rc], n_r.at[rc], mate(rc), core)
    send(norm_all.at[0, 0], norm_all.at[0, 1], n_s.at[4], n_r.at[4], sp, 1 - core)
    for k in [0] + near:
        send_weight(1, 1, k)
    for i in todo:
        forward_weight(0, i)
    for i in order[:4]:
        forward_weight(1, i)
    for rc in (1, 2, 3):
        arrive(norm_all.at[rc, 0], n_s.at[rc], n_r.at[rc])
        j = 4 + rc
        send(norm_all.at[rc, 0], norm_all.at[rc, 1], n_s.at[j], n_r.at[j], sp, 1 - core)
    for i in order[4:6]:
        forward_weight(1, i)
    last_weight(0)
    for rc in range(4):
        arrive(norm_all.at[rc, 1], n_s.at[4 + rc], n_r.at[4 + rc])

    @pl.loop(0, 4 * (cols // tile))
    def _(t):
        rc, c = t // (cols // tile), t % (cols // tile)
        lanes = pl.ds(pl.multiple_of(c * tile, tile), tile)
        tokens = norm_all[rc].reshape(rows, model)
        w = wup[:, :, lanes].reshape(model, tile)
        raised = jnp.dot(tokens, w, preferred_element_type=F32)
        hidden[rc, :, lanes] = jnp.square(jnp.maximum(raised, 0.0)).astype(BF16)

    for i in order[6:]:
        forward_weight(1, i)
    last_weight(1)
    blocks = tile // depth

    def reduce_pair(rc):
        arrive(outs_in.at[rc], o_s.at[rc], o_r.at[rc])
        if rc:

            @pl.loop(0, half // group)
            def _(t):
                rws = pl.ds(pl.multiple_of(t * group, group), group)
                sums[rc - 1, rws] = (
                    outs[rc, 0, rws].astype(F32) + outs_in[rc, rws].astype(F32)
                ).astype(BF16)

            send(sums.at[rc - 1], final_in.at[rc - 1], f_s.at[rc], f_r.at[rc], mate(rc), core)

    before = None
    for rc in (3, 1, 2, 0):

        @pl.loop(0, model // tile)
        def _(t):
            lanes = pl.ds(pl.multiple_of(t * tile, tile), tile)
            w = wdown[pl.ds(t * blocks, blocks)].reshape(tile, cols)
            o = lax.dot_general(hidden[rc], w, NT, preferred_element_type=F32).astype(BF16)
            outs[rc, 0, :, lanes] = o[:half]
            outs[rc, 1, :, lanes] = o[half:]

        send(outs.at[rc, 1], outs_in.at[rc], o_s.at[rc], o_r.at[rc], sp, 1 - core)
        if before is not None:
            reduce_pair(before)
        before = rc
    reduce_pair(0)
    for rc in (1, 2, 3):
        arrive(final_in.at[rc - 1], f_s.at[rc], f_r.at[rc])

    @pl.loop(0, half // group)
    def _(t):
        rws = pl.ds(pl.multiple_of(t * group, group), group)
        total = outs[0, 0, rws].astype(F32) + outs_in[0, rws].astype(F32)
        for rc in range(3):
            total += final_in[rc, rws].astype(F32)
        out_ref[rws] = (mid[rws].astype(F32) + total).astype(BF16)

    for c in sent:
        c.wait_send()


def fused_body(
    queries, keys, values, documents, query_gain, key_gain, out_weight, residual, norm_gain,
    up_weight, down_weight,
):
    rows, heads, width = queries.shape
    n_sp = lax.axis_size("sp")
    model = residual.shape[1]
    depth, cols = up_weight.shape[0], up_weight.shape[1] // 4
    half = rows // 2
    kv_index = lax.axis_index("tp") * heads // (QUERY_HEADS // keys.shape[1])
    positions = lax.axis_index("sp") * rows + jnp.arange(rows, dtype=jnp.int32)
    own_keys = lax.dynamic_index_in_dim(keys, kv_index, 1, keepdims=True)
    own_values = lax.dynamic_index_in_dim(values, kv_index, 1, keepdims=False)
    key_rot = rotate(head_norm(own_keys.astype(F32), key_gain), positions)[:, 0, :].astype(BF16)
    query_rot = rotate(head_norm(queries.astype(F32), query_gain), positions)
    query_rot = (query_rot * (width ** (-0.5) * LOG2E)).astype(BF16)
    kinds = jnp.arange(16, dtype=jnp.int32)
    marks = jnp.where(documents[:, None] == jnp.arange(width)[None, :], APART, 0.0).astype(BF16)
    marks = jnp.broadcast_to(marks[None], (heads, rows, width))
    key_rows = jnp.concatenate(
        [key_rot.T, (kinds[:, None] == documents[None, :]).astype(BF16)], axis=0
    )
    vm = pl.BlockSpec(memory_space=pltpu.VMEM)
    dma = pltpu.SemaphoreType.DMA
    token = (half, model)
    return pl.pallas_call(
        layer_kernel,
        out_shape=jax.ShapeDtypeStruct(token, BF16),
        in_specs=[vm] * 8,
        out_specs=vm,
        scratch_shapes=[
            pltpu.VMEM((n_sp, 2 * width, rows), BF16),
            pltpu.VMEM((n_sp, rows, 2 * width), BF16),
            pltpu.VMEM((rows, heads * width), BF16),
            pltpu.VMEM((n_sp, depth, cols), BF16),
            pltpu.VMEM((n_sp, depth, cols), BF16),
            pltpu.VMEM((2,) + token, BF16),
            pltpu.VMEM(token, BF16),
            pltpu.VMEM(token, BF16),
            pltpu.VMEM((4, 2) + token, BF16),
            pltpu.VMEM((4, rows, cols), BF16),
            pltpu.VMEM((4, 2) + token, BF16),
            pltpu.VMEM((4,) + token, BF16),
            pltpu.VMEM((3,) + token, BF16),
            pltpu.VMEM((3,) + token, BF16),
            dma((n_sp,)), dma((n_sp,)), dma((n_sp,)), dma((n_sp,)),
            dma((2, n_sp)), dma((2, n_sp)), dma((4,)),
            dma, dma, dma((8,)), dma((8,)), dma((4,)), dma((4,)), dma((4,)), dma((4,)),
        ],
        compiler_params=pltpu.CompilerParams(
            collective_id=0, has_side_effects=True, vmem_limit_bytes=60 * 1024 * 1024
        ),
    )(
        jnp.concatenate([query_rot.transpose(1, 0, 2), marks], axis=-1),
        key_rows,
        own_values,
        out_weight,
        residual,
        norm_gain[None, :],
        up_weight,
        down_weight,
    )


def solution(mesh):
    in_specs = (
        P("sp", "tp", None),
        P("sp", None, None),
        P("sp", None, None),
        P("sp"),
        P(),
        P(),
        P("tp", None),
        P("sp", None),
        P(),
        P("sp", "tp"),
        P("sp", "tp"),
    )
    out_specs = P(("sp", "tp"), None)
    fused = mesh.shape["tp"] == 2 and mesh.shape["sp"] == 16
    return jax.shard_map(fused_body if fused else body, mesh=mesh, in_specs=in_specs, out_specs=out_specs, check_vma=False)
```
